512 devices in a mesh: sp: 128 (over z, y, core), tp: 4 (over x).
Axes of the slice: x: 4, y: 8, z: 8, core: 2. Of those that a mesh axis runs over, the one named last changes fastest.
Arguments:
- tokens: bfloat16 [32768, 2048], P(('sp', 'tp')), may hold values from -6 to 6
- norm_gain: float32 [2048], replicated, may hold values from 0.1 to 1.9
- query_weight: bfloat16 [1024, 2048], P('tp', 'sp'), may hold values from -0.088609319 to 0.088609319
- key_weight: bfloat16 [256, 2048], P('tp', 'sp'), may hold values from -0.10628699 to 0.10628699
- value_weight: bfloat16 [256, 2048], P('tp', 'sp'), may hold values from -0.125 to 0.125
- gate_weight: bfloat16 [1024, 2048], P('tp', 'sp'), may hold values from -0.125 to 0.125
- left_weight: bfloat16 [1024, 2048], P('tp', 'sp'), may hold values from -0.125 to 0.125
- input_weight: bfloat16 [1024, 2048], P('tp', 'sp'), may hold values from -0.125 to 0.125
- query_gain: float32 [64], replicated, may hold values from 0.3 to 4.5, as said below
- key_gain: float32 [64], replicated, may hold values from 0.3 to 4.5, as said below
- sink_logit: float32 [16], P('tp'), may hold values from 2 to 7
- conv_weight: float32 [3, 1024], P(None, 'tp'), may hold values from -3 to 3
- out_attention: bfloat16 [1024, 2048], P('tp', 'sp'), may hold values from -0.125 to 0.125
- out_conv: bfloat16 [1024, 2048], P('tp', 'sp'), may hold values from -0.125 to 0.125
Outputs:
- mixed: bfloat16 [32768, 2048], P(('sp', 'tp'))
The draws below stay inside these ranges and needn't reach their ends.
Inputs may be any that keep to these rules, and one draw needn't show every extreme that they name: `query_gain`: positive. `key_gain`: positive.
All inputs are finite; a program needn't handle non-finite values.
Results may differ from the reference program's by a relative error of at most 0.024.
Values may be sent and summed in bfloat16 or wider, within the bound.
No kernel may reach another device: no remote copies, remote signals or barrier semaphores. Data moves between devices by JAX's collectives and lax.ppermute only.
A program may use at most 64 MiB of HBM per device.

```python
import jax
import jax.numpy as jnp
from jax import lax

D = 2048
HEAD_DIM = 64
Q_HEADS = 16
KV_HEADS = 4
CONV_CH = 1024
WINDOW = 128
BLOCK = 128
TOKENS = 32768
N_TP = 4


def shared_query(key):
    return jnp.clip(jax.random.normal(jax.random.fold_in(key, 101), (Q_HEADS * HEAD_DIM, D), jnp.float32), -4.0, 4.0) * D ** (-0.5)


def draw_query_weight(key, part):
    return shared_query(key).astype(jnp.bfloat16)


def draw_key_weight(key, part):
    noise = jnp.clip(jax.random.normal(jax.random.fold_in(key, 102), (KV_HEADS * HEAD_DIM, D), jnp.float32), -4.0, 4.0) * D ** (-0.5)
    result = noise
    return result.astype(jnp.bfloat16)


def draw_query_gain(key, part):
    result = jax.random.uniform(jax.random.fold_in(key, 103), (HEAD_DIM,), jnp.float32, 0.3, 1.9)
    return result


def draw_key_gain(key, part):
    result = jax.random.uniform(jax.random.fold_in(key, 104), (HEAD_DIM,), jnp.float32, 0.3, 1.9)
    return result


def level_of(rng, shape, cuts, least, top_value):
    def one(axis_at, parts):
        draws = jax.random.uniform(jax.random.fold_in(jax.random.fold_in(rng, 6), axis_at), (parts,), jnp.float32, least / len(cuts), top_value / len(cuts))
        return jnp.repeat(jnp.exp(draws), shape[axis_at] // parts).reshape((-1,) + (1,) * (len(shape) - axis_at - 1))

    loudness = one(*cuts[0])
    for cut in cuts[1:]:
        loudness = loudness * one(*cut)
    return loudness


def centred(own_key, extent, deviation, limit, split=(), held_as=jnp.bfloat16):
    level = level_of(own_key, extent, split, -0.22, 0.18) if split else 1.0
    drawn = jax.random.normal(own_key, extent, jnp.float32) * deviation * level
    return jnp.minimum(jnp.maximum(drawn, -limit), limit).astype(held_as)


def setup_inputs(seed: int = 0) -> dict:
    splits = jax.random.split(jax.random.key(seed), 15)
    return {
        "tokens": centred(splits[0], (TOKENS, D), 1.0, 6.0, ((0, 512),)),
        "norm_gain": jnp.clip(1.0 + 0.18 * jax.random.normal(splits[1], (D,), jnp.float32), 0.1, 1.9),
        "query_weight": draw_query_weight(jax.random.fold_in(splits[14], 71), 0),
        "key_weight": draw_key_weight(jax.random.fold_in(splits[14], 71), 0),
        "value_weight": centred(splits[4], (KV_HEADS * HEAD_DIM, D), D ** -0.5, 0.125, ((0, 4), (1, 128))),
        "gate_weight": centred(splits[5], (CONV_CH, D), D ** -0.5, 0.125, ((0, 4), (1, 128))),
        "left_weight": centred(splits[6], (CONV_CH, D), D ** -0.5, 0.125, ((0, 4), (1, 128))),
        "input_weight": centred(splits[7], (CONV_CH, D), D ** -0.5, 0.125, ((0, 4), (1, 128))),
        "query_gain": draw_query_gain(jax.random.fold_in(splits[14], 71), 0),
        "key_gain": draw_key_gain(jax.random.fold_in(splits[14], 71), 0),
        "sink_logit": jnp.clip(2.0 + 5.0 * jax.random.uniform(splits[10], (Q_HEADS,), jnp.float32) ** level_of(splits[10], (Q_HEADS,), ((0, 4),), -0.2, 0.2), 2.0, 7.0),
        "conv_weight": centred(splits[11], (3, CONV_CH), 0.6, 3.0, ((1, 4),), jnp.float32),
        "out_attention": centred(splits[12], (Q_HEADS * HEAD_DIM, D), (Q_HEADS * HEAD_DIM + CONV_CH) ** -0.5, 0.125, ((0, 4), (1, 128))),
        "out_conv": centred(splits[13], (CONV_CH, D), (Q_HEADS * HEAD_DIM + CONV_CH) ** -0.5, 0.125, ((0, 4), (1, 128))),
    }


EPS = 1e-06
ROPE_BASE = 10000.0
NEG_FILL = -1e+30

def normalize(values, gain):
    return values * lax.rsqrt(lax.optimization_barrier(jnp.mean(values * values, axis=-1, keepdims=True)) + EPS) * gain

def rotate(values, positions):
    half = values.shape[-1] // 2
    freq = ROPE_BASE ** (-jnp.arange(half, dtype=jnp.float32) / half)
    angle = positions[:, None] * freq
    cosine = jnp.cos(angle)[:, None, :]
    sine = jnp.sin(angle)[:, None, :]
    first = values[..., :half]
    second = values[..., half:]
    return jnp.concatenate([first * cosine - second * sine, second * cosine + first * sine], axis=-1)

def project(rows, weight):
    return lax.dot_general(rows, weight, (((1,), (1,)), ((), ())), preferred_element_type=jnp.float32).astype(jnp.bfloat16)

def reference(tokens, norm_gain, query_weight, key_weight, value_weight, gate_weight, left_weight, input_weight, query_gain, key_gain, sink_logit, conv_weight, out_attention, out_conv):
    count = tokens.shape[0]
    normed = normalize(tokens.astype(jnp.float32), norm_gain).astype(jnp.bfloat16)
    query = project(normed, query_weight).reshape(count, Q_HEADS, HEAD_DIM)
    keys = project(normed, key_weight).reshape(count, KV_HEADS, HEAD_DIM)
    values = project(normed, value_weight).reshape(count, KV_HEADS, HEAD_DIM)
    gate = project(normed, gate_weight)
    left = project(normed, left_weight)
    inputs = project(normed, input_weight)
    positions = jnp.arange(count, dtype=jnp.float32)
    query_rot = rotate(normalize(query.astype(jnp.float32), query_gain), positions).astype(jnp.bfloat16)
    key_rot = rotate(normalize(keys.astype(jnp.float32), key_gain), positions).astype(jnp.bfloat16)
    group = Q_HEADS // KV_HEADS
    span = BLOCK + 2 * WINDOW
    padded_keys = jnp.pad(key_rot, ((WINDOW, WINDOW), (0, 0), (0, 0)))
    padded_values = jnp.pad(values, ((WINDOW, WINDOW), (0, 0), (0, 0)))
    nblocks = count // BLOCK
    shaped = query_rot.reshape(nblocks, BLOCK, KV_HEADS, group, HEAD_DIM)
    sinks = sink_logit.reshape(KV_HEADS, group)[:, :, None]

    def one_block(packed):
        block_index, query_block = packed
        begin = block_index * BLOCK
        key_block = lax.dynamic_slice_in_dim(padded_keys, begin, span, 0)
        value_block = lax.dynamic_slice_in_dim(padded_values, begin, span, 0)
        scores = jnp.einsum('qkgd,nkd->kgqn', query_block.astype(jnp.float32), key_block.astype(jnp.float32)) * HEAD_DIM ** (-0.5)
        query_pos = begin + jnp.arange(BLOCK, dtype=jnp.int32)
        key_pos = begin - WINDOW + jnp.arange(span, dtype=jnp.int32)
        allowed = (jnp.abs(query_pos[:, None] - key_pos[None, :]) <= WINDOW) & (key_pos >= 0)[None, :] & (key_pos < count)[None, :]
        scores = jnp.where(allowed, scores, NEG_FILL)
        top = jnp.maximum(lax.optimization_barrier(jnp.max(scores, axis=-1)), sinks)
        expo = jnp.exp(scores - top[..., None])
        total = lax.optimization_barrier(jnp.sum(expo, axis=-1)) + jnp.exp(sinks - top)
        weights = (expo / total[..., None]).astype(jnp.bfloat16)
        return jnp.einsum('kgqn,nkd->qkgd', weights.astype(jnp.float32), value_block.astype(jnp.float32)).astype(jnp.bfloat16)
    attended = lax.map(one_block, (jnp.arange(nblocks, dtype=jnp.int32), shaped)).reshape(count, Q_HEADS * HEAD_DIM)
    product = (left.astype(jnp.float32) * inputs.astype(jnp.float32)).astype(jnp.bfloat16)
    padded = jnp.pad(product.astype(jnp.float32), ((1, 1), (0, 0)))
    convolved = conv_weight[0] * padded[:-2] + conv_weight[1] * padded[1:-1] + conv_weight[2] * padded[2:]
    gated = (gate.astype(jnp.float32) * convolved).astype(jnp.bfloat16)
    attn_width = Q_HEADS * HEAD_DIM // N_TP
    conv_width = CONV_CH // N_TP
    summed = jnp.zeros((count, D), jnp.float32)
    for place in range(N_TP):
        partial_sum = jnp.dot(attended[:, place * attn_width:(place + 1) * attn_width], out_attention[place * attn_width:(place + 1) * attn_width], preferred_element_type=jnp.float32)
        partial_sum = partial_sum + jnp.dot(gated[:, place * conv_width:(place + 1) * conv_width], out_conv[place * conv_width:(place + 1) * conv_width], preferred_element_type=jnp.float32)
        summed = summed + partial_sum.astype(jnp.bfloat16).astype(jnp.float32)
    return summed.astype(jnp.bfloat16)
```

```python
import jax
import jax.numpy as jnp
import numpy as np
from jax import lax
from jax.experimental import pallas as pl
from jax.experimental.pallas import tpu as pltpu
from jax.sharding import PartitionSpec as P


HEAD = 64
HALF = HEAD // 2
WINDOW = 128
BLOCK = 128
EPS = 1e-06
ROPE_BASE = 10000.0
NEG_FILL = -1e30
RING = 8
TP = 4
CHIPS = RING * RING
LOCAL = 64
CHIP_TOKENS = 2 * TP * LOCAL
ROWS = CHIP_TOKENS + 2 * WINDOW
PROJ = 640
OUTW = 256
WIDTH = PROJ + OUTW


def sp_of(z, y, c):
    return (z * RING + y) * 2 + c


def even_partner(pos):
    return pos ^ 1


def odd_partner(pos):
    return (pos - 1) % RING if pos % 2 == 0 else (pos + 1) % RING


def matching(partner):
    pairs = []
    for z in range(RING):
        for y in range(RING):
            pairs.append((sp_of(z, y, 0), sp_of(z, partner(y), 0)))
            pairs.append((sp_of(z, y, 1), sp_of(partner(z), y, 1)))
    return pairs


EVEN = matching(even_partner)
ODD = matching(odd_partner)
SWAP = [(2 * k + c, 2 * k + 1 - c) for k in range(CHIPS) for c in range(2)]
GROUPS = [[sp_of(z, y, 0) for z in range(RING)] for y in range(RING)] + [
    [sp_of(z, y, 1) for y in range(RING)] for z in range(RING)
]
HALOS = [
    [
        ((2 * k + 1) * TP + x, (2 * k + 2 + c) * TP + x) for k in range(CHIPS - 1) for x in (2, 3)
    ]
    + [((2 * k + 2) * TP + x, (2 * k + c) * TP + x) for k in range(CHIPS - 1) for x in (0, 1)]
    for c in range(2)
]
PART = LOCAL // 2
SHARE = LOCAL + PART
ANGLES = np.tile(ROPE_BASE ** (-np.arange(HALF) / HALF), 128 // HALF).astype(np.float32)
VMEM = pl.BlockSpec(memory_space=pltpu.VMEM)
SMEM = pl.BlockSpec(memory_space=pltpu.SMEM)


def columns_kernel(q, k, v, g, l, i, oa, oc, out):
    at = 0
    for c in range(2):
        for ref in (q, k, v, g, l, i, oa, oc):
            if ref.shape[1] == HEAD:
                width, first = HEAD, 0
            else:
                width, first = 128, c * 128
            out[:, at : at + width] = ref[:, first : first + width]
            at += width


def columns(weights):
    return pl.pallas_call(
        columns_kernel,
        out_shape=jax.ShapeDtypeStruct((weights[0].shape[1], 2 * WIDTH), jnp.bfloat16),
        in_specs=[VMEM] * len(weights),
        out_specs=VMEM,
        name="columns",
    )(*[w.T for w in weights])


def copies_kernel(where_ref, mine_ref, got_ref, out):
    core = where_ref[2]
    for to, ref in enumerate((mine_ref, got_ref)):
        block = jnp.where(core == 0, ref[:, :WIDTH], ref[:, WIDTH:])
        for k in range(RING):
            out[k, to * 16 : (to + 1) * 16, :] = block


def copies(where, mine, got):
    return pl.pallas_call(
        copies_kernel,
        out_shape=jax.ShapeDtypeStruct((RING, 32, WIDTH), jnp.bfloat16),
        in_specs=[SMEM, VMEM, VMEM],
        out_specs=VMEM,
        name="copies",
    )(where, mine, got)


def rows_kernel(normed, rim0, rim1, out):
    rim = rim0[...] + rim1[...]
    for x in range(TP):
        out[x, :LOCAL, :] = normed[...]
        out[x, LOCAL:, :] = rim


def row_copies(normed, rim0, rim1):
    return pl.pallas_call(
        rows_kernel,
        out_shape=jax.ShapeDtypeStruct((TP, SHARE, normed.shape[1]), jnp.bfloat16),
        in_specs=[VMEM] * 3,
        out_specs=VMEM,
        name="rows",
    )(normed, rim0, rim1)


def gathered_weights(where, mine):
    got = lax.ppermute(mine, "sp", SWAP)
    blocks = copies(where, mine, got)
    own = lax.all_to_all(blocks, "sp", 0, 0, axis_index_groups=GROUPS, tiled=True)
    own = own.reshape(RING * 32, WIDTH)
    e1 = lax.ppermute(own, "sp", EVEN)
    o1 = lax.ppermute(own, "sp", ODD)
    o2 = lax.ppermute(e1, "sp", ODD)
    e2 = lax.ppermute(o1, "sp", EVEN)
    e3 = lax.ppermute(o2, "sp", EVEN)
    o3 = lax.ppermute(e2, "sp", ODD)
    o4 = lax.ppermute(e3, "sp", ODD)
    return own, e1, o1, e2, o2, e3, o3, o4


def norm_kernel(x_ref, gain_ref, normed, part0, part1):
    wide = x_ref[...].astype(jnp.float32)
    mean = jnp.mean(wide * wide, axis=-1, keepdims=True)
    value = (wide * lax.rsqrt(mean + EPS) * gain_ref[...]).astype(jnp.bfloat16)
    normed[...] = value
    part0[...] = value[:PART]
    part1[...] = value[PART:]


def normalized(tokens, norm_gain):
    rows, features = tokens.shape
    part = jax.ShapeDtypeStruct((PART, features), jnp.bfloat16)
    return pl.pallas_call(
        norm_kernel,
        out_shape=(jax.ShapeDtypeStruct((rows, features), jnp.bfloat16), part, part),
        in_specs=[VMEM] * 2,
        out_specs=(VMEM,) * 3,
        name="norm",
    )(tokens, norm_gain[None])


def gathered_tokens(normed, part0, part1):
    both = ("sp", "tp")
    rim0 = lax.ppermute(part0, both, HALOS[0])
    rim1 = lax.ppermute(part1, both, HALOS[1])
    sent = row_copies(normed, rim0, rim1)
    mine = lax.all_to_all(sent, "tp", 0, 0, tiled=True).reshape(TP * SHARE, -1)
    return mine, lax.ppermute(mine, "sp", SWAP)


def layer_kernel(
    where_ref,
    sink_ref,
    x_ref,
    x2_ref,
    own,
    e1,
    o1,
    e2,
    o2,
    e3,
    o3,
    o4,
    cos_ref,
    sin_ref,
    qg_ref,
    kg_ref,
    conv_ref,
    kept_ref,
    sent_ref,
    w_s,
    p_s,
    kk_s,
    vv_s,
    prod_s,
    act_s,
):
    pos, sgn, core, chip = where_ref[0], where_ref[1], where_ref[2], where_ref[3]

    def place(piece, steps):
        at = lax.rem(pos + sgn * steps + 2 * RING, RING)
        for j in range(RING):
            start = jnp.where(core == 0, j * 256 + at * 32, at * 256 + j * 32)
            for h in range(2):
                to = start + 16 * (core if h == 0 else 1 - core)
                w_s[pl.ds(pl.multiple_of(to, 16), 16), :] = piece[
                    j * 32 + h * 16 : j * 32 + h * 16 + 16, :
                ]

    place(own, 0)
    place(e1, 1)
    place(o1, -1)
    place(e2, 2)
    place(o2, -2)
    place(e3, 3)
    place(o3, -3)
    place(o4, -4)

    for ref, c in ((x_ref, core), (x2_ref, 1 - core)):
        tokens = ref[...]
        for lo, hi in ((0, 256), (256, 512), (512, PROJ)):
            part = jnp.dot(tokens, w_s[:, lo:hi], preferred_element_type=jnp.float32).astype(
                jnp.bfloat16
            )
            for x in range(TP):
                base = x * SHARE
                to = WINDOW + x * LOCAL + c * (TP * LOCAL)
                p_s[pl.ds(pl.multiple_of(to, LOCAL), LOCAL), lo:hi] = part[base : base + LOCAL]
                to = ((x - 2) * LOCAL if x >= 2 else WINDOW + CHIP_TOKENS + x * LOCAL) + c * PART
                p_s[pl.ds(pl.multiple_of(to, PART), PART), lo:hi] = part[base + LOCAL : base + SHARE]

    def gain_rows(ref, scale):
        gain = jnp.concatenate([ref[...], ref[...]], axis=1) * scale
        lane = lax.rem(lax.broadcasted_iota(jnp.int32, gain.shape, 1), HEAD)
        low = pltpu.roll(gain, 128 - HALF, 1)
        return gain, jnp.where(lane < HALF, -low, pltpu.roll(gain, HALF, 1))

    query_gain = gain_rows(qg_ref, HEAD ** (-0.5))
    key_gain = gain_rows(kg_ref, 1.0)

    def rotated(value, at, gain, crossed_gain):
        lane = lax.broadcasted_iota(jnp.int32, value.shape, 1)
        low = lane < HEAD
        square = value * value
        mean0 = jnp.sum(jnp.where(low, square, 0.0), axis=-1, keepdims=True) * (1.0 / HEAD)
        mean1 = jnp.sum(jnp.where(low, 0.0, square), axis=-1, keepdims=True) * (1.0 / HEAD)
        scaled = value * jnp.where(low, lax.rsqrt(mean0 + EPS), lax.rsqrt(mean1 + EPS))
        crossed = jnp.where(
            lax.rem(lane, HEAD) < HALF,
            pltpu.roll(scaled, 2 * HEAD - HALF, 1),
            pltpu.roll(scaled, HALF, 1),
        )
        cosine = cos_ref[at : at + BLOCK, :]
        sine = sin_ref[at : at + BLOCK, :]
        return scaled * (cosine * gain) + crossed * (sine * crossed_gain)

    for at in range(0, ROWS, BLOCK):
        kv = p_s[at : at + BLOCK, 128:256].astype(jnp.float32)
        lane = lax.broadcasted_iota(jnp.int32, kv.shape, 1)
        key = rotated(kv, at, *key_gain)
        kk_s[at : at + BLOCK, :] = jnp.where(lane < HEAD, key, pltpu.roll(key, HEAD, 1)).astype(
            jnp.bfloat16
        )
        vv_s[at : at + BLOCK, :] = jnp.where(lane < HEAD, pltpu.roll(kv, HEAD, 1), kv).astype(
            jnp.bfloat16
        )
        prod_s[at : at + BLOCK, :] = (
            (
                p_s[at : at + BLOCK, 384:512].astype(jnp.float32)
                * p_s[at : at + BLOCK, 512:640].astype(jnp.float32)
            )
            .astype(jnp.bfloat16)
            .astype(jnp.float32)
        )

    conv = jnp.where(core == 0, conv_ref[:, :128], conv_ref[:, 128:])
    for at in range(0, CHIP_TOKENS, BLOCK):
        rows = slice(at + WINDOW, at + WINDOW + BLOCK)
        query = rotated(p_s[rows, 0:128].astype(jnp.float32), at + WINDOW, *query_gain)
        low = lax.broadcasted_iota(jnp.int32, query.shape, 1) < HEAD
        keys = kk_s[at : at + 3 * BLOCK, :]
        values = vv_s[at : at + 3 * BLOCK, :]
        shape = (BLOCK, 3 * BLOCK)
        q_at = lax.broadcasted_iota(jnp.int32, shape, 0)
        k_at = lax.broadcasted_iota(jnp.int32, shape, 1) - WINDOW
        k_pos = k_at + (chip * CHIP_TOKENS + at)
        allowed = (
            (jnp.abs(q_at - k_at) <= WINDOW) & (k_pos >= 0) & (k_pos < CHIPS * CHIP_TOKENS)
        )
        outs = []
        for head in range(2):
            q_head = jnp.where(low if head == 0 else ~low, query, 0.0).astype(jnp.bfloat16)
            scores = lax.dot_general(
                q_head, keys, (((1,), (1,)), ((), ())), preferred_element_type=jnp.float32
            )
            scores = jnp.where(allowed, scores, NEG_FILL)
            sink = sink_ref[2 * core + head]
            top = jnp.maximum(jnp.max(scores, axis=-1, keepdims=True), sink)
            expo = jnp.exp(scores - top)
            total = jnp.sum(expo, axis=-1, keepdims=True) + jnp.exp(sink - top)
            weights = (expo * (1.0 / total)).astype(jnp.bfloat16)
            outs.append(jnp.dot(weights, values, preferred_element_type=jnp.float32))
        act_s[at : at + BLOCK, 0:128] = jnp.where(low, outs[0], outs[1]).astype(jnp.bfloat16)
        lo = at + WINDOW
        mixed = (
            conv[0:1, :] * prod_s[lo - 1 : lo - 1 + BLOCK, :]
            + conv[1:2, :] * prod_s[lo : lo + BLOCK, :]
            + conv[2:3, :] * prod_s[lo + 1 : lo + 1 + BLOCK, :]
        )
        act_s[at : at + BLOCK, 128:256] = (p_s[rows, 256:384].astype(jnp.float32) * mixed).astype(
            jnp.bfloat16
        )

    half = CHIP_TOKENS // 2
    for ref, c in ((sent_ref, 1 - core), (kept_ref, core)):
        for at in range(0, half, BLOCK):
            ref[at : at + BLOCK, :] = lax.dot_general(
                act_s[pl.ds(pl.multiple_of(c * half + at, BLOCK), BLOCK), :],
                w_s[:, PROJ:],
                (((1,), (1,)), ((), ())),
                preferred_element_type=jnp.float32,
            ).astype(jnp.bfloat16)


def run_layer(where, sinks, tokens, pieces, tables, conv):
    features = tokens[0].shape[-1]
    shape = jax.ShapeDtypeStruct((CHIP_TOKENS // 2, features), jnp.bfloat16)
    return pl.pallas_call(
        layer_kernel,
        out_shape=(shape, shape),
        in_specs=[SMEM, SMEM] + [VMEM] * (len(tokens) + len(pieces) + len(tables) + 1),
        out_specs=(VMEM, VMEM),
        scratch_shapes=[
            pltpu.VMEM((features, WIDTH), jnp.bfloat16),
            pltpu.VMEM((ROWS, PROJ), jnp.bfloat16),
            pltpu.VMEM((ROWS, 128), jnp.bfloat16),
            pltpu.VMEM((ROWS, 128), jnp.bfloat16),
            pltpu.VMEM((ROWS, 128), jnp.float32),
            pltpu.VMEM((CHIP_TOKENS, 256), jnp.bfloat16),
        ],
        compiler_params=pltpu.CompilerParams(vmem_limit_bytes=48 * 1024 * 1024),
        name="layer",
    )(where, sinks, *tokens, *pieces, *tables, conv)


def per_device(
    tokens,
    norm_gain,
    query_weight,
    key_weight,
    value_weight,
    gate_weight,
    left_weight,
    input_weight,
    query_gain,
    key_gain,
    sink_logit,
    conv_weight,
    out_attention,
    out_conv,
):
    sp_place = lax.axis_index("sp").astype(jnp.int32)
    core = lax.rem(sp_place, 2)
    chip = sp_place // 2
    y = lax.rem(chip, RING)
    z = chip // RING
    pos = jnp.where(core == 0, y, z)
    sgn = 1 - 2 * lax.rem(pos, 2)

    where = jnp.stack([pos, sgn, core, chip])
    mine = columns(
        (
            query_weight,
            key_weight,
            value_weight,
            gate_weight,
            left_weight,
            input_weight,
            out_attention,
            out_conv,
        )
    )
    rows = normalized(tokens, norm_gain)
    gathered = gathered_tokens(*rows)
    pieces = gathered_weights(where, mine)

    positions = (chip * CHIP_TOKENS - WINDOW + jnp.arange(ROWS, dtype=jnp.int32)).astype(
        jnp.float32
    )
    angle = positions[:, None] * ANGLES
    tables = (jnp.cos(angle), jnp.sin(angle), query_gain[None], key_gain[None])
    kept, sent = run_layer(where, sink_logit, gathered, pieces, tables, conv_weight)

    arrived = lax.ppermute(sent, "sp", SWAP)
    group = (kept.astype(jnp.float32) + arrived.astype(jnp.float32)).astype(jnp.bfloat16)
    blocks = lax.all_to_all(group.reshape(TP, LOCAL, -1), "tp", 0, 0, tiled=True)
    return blocks.astype(jnp.float32).sum(axis=0).astype(jnp.bfloat16)


def solution(mesh):
    in_specs = (
        P(("sp", "tp"), None),
        P(),
        P("tp", "sp"),
        P("tp", "sp"),
        P("tp", "sp"),
        P("tp", "sp"),
        P("tp", "sp"),
        P("tp", "sp"),
        P(),
        P(),
        P("tp"),
        P(None, "tp"),
        P("tp", "sp"),
        P("tp", "sp"),
    )
    out_specs = P(("sp", "tp"), None)

    return jax.shard_map(
        per_device, mesh=mesh, in_specs=in_specs, out_specs=out_specs, check_vma=False
    )
```

```python
import jax
import jax.numpy as jnp
import numpy as np
from jax import lax
from jax.experimental import pallas as pl
from jax.experimental.pallas import tpu as pltpu
from jax.sharding import PartitionSpec as P


HEAD = 64
HALF = HEAD // 2
WINDOW = 128
BLOCK = 128
EPS = 1e-06
ROPE_BASE = 10000.0
NEG_FILL = -1e30
RING = 8
TP = 4
CHIPS = RING * RING
SP = 2 * CHIPS
LOCAL = 64
MAIN = TP * LOCAL
ROWS = MAIN + 2 * WINDOW
SHARE = 2 * LOCAL
PROJ = 1152
WIDTH = PROJ + 512


def sp_of(z, y, c):
    return (z * RING + y) * 2 + c


def even_partner(pos):
    return pos ^ 1


def odd_partner(pos):
    return (pos - 1) % RING if pos % 2 == 0 else (pos + 1) % RING


def matching(partner):
    pairs = []
    for z in range(RING):
        for y in range(RING):
            pairs.append((sp_of(z, y, 0), sp_of(z, partner(y), 0)))
            pairs.append((sp_of(z, y, 1), sp_of(partner(z), y, 1)))
    return pairs


EVEN = matching(even_partner)
ODD = matching(odd_partner)
SWAP = [(2 * k + c, 2 * k + 1 - c) for k in range(CHIPS) for c in range(2)]
GROUPS = [[sp_of(z, y, 0) for z in range(RING)] for y in range(RING)] + [
    [sp_of(z, y, 1) for y in range(RING)] for z in range(RING)
]
HALO = [(s * TP + x, (s + 1) * TP + x) for s in range(SP - 1) for x in (2, 3)] + [
    ((s + 1) * TP + x, s * TP + x) for s in range(SP - 1) for x in (0, 1)
]
MIB = 1024 * 1024
ANGLES = np.tile(ROPE_BASE ** (-np.arange(HALF) / HALF), 128 // HALF).astype(np.float32)
VMEM = pl.BlockSpec(memory_space=pltpu.VMEM)
SMEM = pl.BlockSpec(memory_space=pltpu.SMEM)


def copies_kernel(*refs):
    *weights, out = refs
    at = 0
    for ref in weights:
        width = ref.shape[1]
        for k in range(RING):
            out[k, :, at : at + width] = ref[...]
        at += width


def copies(weights):
    return pl.pallas_call(
        copies_kernel,
        out_shape=jax.ShapeDtypeStruct((RING, weights[0].shape[1], WIDTH), jnp.bfloat16),
        in_specs=[VMEM] * len(weights),
        out_specs=VMEM,
        name="copies",
    )(*[w.T for w in weights])


def rows_kernel(normed, rim, out):
    for x in range(TP):
        out[x, :LOCAL, :] = normed[...]
        out[x, LOCAL:, :] = rim[...]


def row_copies(normed, rim):
    return pl.pallas_call(
        rows_kernel,
        out_shape=jax.ShapeDtypeStruct((TP, SHARE, normed.shape[1]), jnp.bfloat16),
        in_specs=[VMEM] * 2,
        out_specs=VMEM,
        compiler_params=pltpu.CompilerParams(vmem_limit_bytes=8 * MIB),
    name="rows",
    )(normed, rim)


def gathered_weights(weights):
    blocks = copies(weights)
    own = lax.all_to_all(blocks, "sp", 0, 0, axis_index_groups=GROUPS, tiled=True)
    own = own.reshape(-1, WIDTH)
    e1 = lax.ppermute(own, "sp", EVEN)
    o1 = lax.ppermute(own, "sp", ODD)
    o2 = lax.ppermute(e1, "sp", ODD)
    e2 = lax.ppermute(o1, "sp", EVEN)
    e3 = lax.ppermute(o2, "sp", EVEN)
    o3 = lax.ppermute(e2, "sp", ODD)
    o4 = lax.ppermute(e3, "sp", ODD)
    first = packed((own, e1, o1, o2))
    second = packed((e2, e3, o3))
    kept = (first, second, o4)
    return kept + tuple(lax.ppermute(p, "sp", SWAP) for p in kept)


def packed(pieces):
    def body(*refs):
        *sources, out = refs
        for k, ref in enumerate(sources):
            out[k * 128 : (k + 1) * 128, :] = ref[...]

    return pl.pallas_call(
        body,
        out_shape=jax.ShapeDtypeStruct((128 * len(pieces), WIDTH), jnp.bfloat16),
        in_specs=[VMEM] * len(pieces),
        out_specs=VMEM,
        compiler_params=pltpu.CompilerParams(vmem_limit_bytes=8 * MIB),
    )(*pieces)


def norm_kernel(x_ref, gain_ref, normed):
    wide = x_ref[...].astype(jnp.float32)
    mean = jnp.mean(wide * wide, axis=-1, keepdims=True)
    normed[...] = (wide * lax.rsqrt(mean + EPS) * gain_ref[...]).astype(jnp.bfloat16)


def normalized(tokens, norm_gain):
    return pl.pallas_call(
        norm_kernel,
        out_shape=jax.ShapeDtypeStruct(tokens.shape, jnp.bfloat16),
        in_specs=[VMEM] * 2,
        out_specs=VMEM,
        name="norm",
    )(tokens, norm_gain[None])


def gathered_tokens(normed):
    rim = lax.ppermute(normed, ("sp", "tp"), HALO)
    sent = row_copies(normed, rim)
    return lax.all_to_all(sent, "tp", 0, 0, tiled=True)


PIECE_STEPS = (0, 1, -1, -2, 2, 3, -3, -4)


def layer_kernel(where_ref, sink_ref, x_ref, *refs):
    pieces = []
    for first, second, third in (refs[:3], refs[3:6]):
        pieces += [(first, k * 128) for k in range(4)]
        pieces += [(second, k * 128) for k in range(3)] + [(third, 0)]
    cos_ref, sin_ref, qg_ref, kg_ref, conv_ref, out_ref = refs[6:12]
    w_s, p_s, kk_s, vv_s, prod_s, act_s = refs[12:]
    core, y, z, place = where_ref[0], where_ref[1], where_ref[2], where_ref[3]

    for k, (piece, base) in enumerate(pieces):
        owner = core if k < 8 else 1 - core
        pos = jnp.where(owner == 0, y, z)
        sgn = 1 - 2 * lax.rem(pos, 2)
        at = lax.rem(pos + sgn * PIECE_STEPS[k % 8] + 2 * RING, RING)
        for j in range(RING):
            to = jnp.where(owner == 0, j * 256 + at * 32, at * 256 + j * 32 + 16)
            w_s[pl.ds(pl.multiple_of(to, 16), 16), :] = piece[
                base + j * 16 : base + (j + 1) * 16, :
            ]

    features = x_ref.shape[-1]
    main = x_ref[:, :LOCAL, :].reshape(MAIN, features)
    rim = x_ref[:, LOCAL:, :].reshape(MAIN, features)
    for lo in range(0, PROJ, 128):
        cols = slice(lo, lo + 128)
        part = jnp.dot(main, w_s[:, cols], preferred_element_type=jnp.float32)
        p_s[WINDOW : WINDOW + MAIN, cols] = part.astype(jnp.bfloat16)
        if lo < 256 or 384 <= lo < 640:
            continue
        part = jnp.dot(rim, w_s[:, cols], preferred_element_type=jnp.float32).astype(jnp.bfloat16)
        p_s[:WINDOW, cols] = part[WINDOW:]
        p_s[WINDOW + MAIN :, cols] = part[:WINDOW]

    def gain_rows(ref, scale):
        gain = jnp.concatenate([ref[...], ref[...]], axis=1) * scale
        lane = lax.rem(lax.broadcasted_iota(jnp.int32, gain.shape, 1), HEAD)
        low = pltpu.roll(gain, 128 - HALF, 1)
        return gain, jnp.where(lane < HALF, -low, pltpu.roll(gain, HALF, 1))

    query_gain = gain_rows(qg_ref, HEAD ** (-0.5))
    key_gain = gain_rows(kg_ref, 1.0)

    def rotated(value, at, gain, crossed_gain):
        lane = lax.broadcasted_iota(jnp.int32, value.shape, 1)
        low = lane < HEAD
        square = value * value
        mean0 = jnp.sum(jnp.where(low, square, 0.0), axis=-1, keepdims=True) * (1.0 / HEAD)
        mean1 = jnp.sum(jnp.where(low, 0.0, square), axis=-1, keepdims=True) * (1.0 / HEAD)
        scaled = value * jnp.where(low, lax.rsqrt(mean0 + EPS), lax.rsqrt(mean1 + EPS))
        crossed = jnp.where(
            lax.rem(lane, HEAD) < HALF,
            pltpu.roll(scaled, 2 * HEAD - HALF, 1),
            pltpu.roll(scaled, HALF, 1),
        )
        cosine = cos_ref[at : at + BLOCK, :]
        sine = sin_ref[at : at + BLOCK, :]
        return scaled * (cosine * gain) + crossed * (sine * crossed_gain)

    for at in range(0, ROWS, BLOCK):
        kv = p_s[at : at + BLOCK, 256:384].astype(jnp.float32)
        lane = lax.broadcasted_iota(jnp.int32, kv.shape, 1)
        key = rotated(kv, at, *key_gain)
        kk_s[at : at + BLOCK, :] = jnp.where(lane < HEAD, key, pltpu.roll(key, HEAD, 1)).astype(
            jnp.bfloat16
        )
        vv_s[at : at + BLOCK, :] = jnp.where(lane < HEAD, pltpu.roll(kv, HEAD, 1), kv).astype(
            jnp.bfloat16
        )
        prod_s[at : at + BLOCK, :] = (
            (
                p_s[at : at + BLOCK, 640:896].astype(jnp.float32)
                * p_s[at : at + BLOCK, 896:1152].astype(jnp.float32)
            )
            .astype(jnp.bfloat16)
            .astype(jnp.float32)
        )

    for at in range(0, MAIN, BLOCK):
        rows = slice(at + WINDOW, at + WINDOW + BLOCK)
        keys = kk_s[at : at + 3 * BLOCK, :]
        values = vv_s[at : at + 3 * BLOCK, :]
        shape = (BLOCK, 3 * BLOCK)
        q_at = lax.broadcasted_iota(jnp.int32, shape, 0)
        k_at = lax.broadcasted_iota(jnp.int32, shape, 1) - WINDOW
        k_pos = k_at + (place * MAIN + at)
        allowed = (jnp.abs(q_at - k_at) <= WINDOW) & (k_pos >= 0) & (k_pos < SP * MAIN)
        for pair in range(2):
            lanes = slice(pair * 128, (pair + 1) * 128)
            query = rotated(p_s[rows, lanes].astype(jnp.float32), at + WINDOW, *query_gain)
            low = lax.broadcasted_iota(jnp.int32, query.shape, 1) < HEAD
            outs = []
            for head in range(2):
                q_head = jnp.where(low if head == 0 else ~low, query, 0.0).astype(jnp.bfloat16)
                scores = lax.dot_general(
                    q_head, keys, (((1,), (1,)), ((), ())), preferred_element_type=jnp.float32
                )
                scores = jnp.where(allowed, scores, NEG_FILL)
                sink = sink_ref[2 * pair + head]
                top = jnp.maximum(jnp.max(scores, axis=-1, keepdims=True), sink)
                expo = jnp.exp(scores - top)
                total = jnp.sum(expo, axis=-1, keepdims=True) + jnp.exp(sink - top)
                weights = (expo * (1.0 / total)).astype(jnp.bfloat16)
                outs.append(jnp.dot(weights, values, preferred_element_type=jnp.float32))
            act_s[at : at + BLOCK, lanes] = jnp.where(low, outs[0], outs[1]).astype(jnp.bfloat16)
        lo = at + WINDOW
        mixed = (
            conv_ref[0:1, :] * prod_s[lo - 1 : lo - 1 + BLOCK, :]
            + conv_ref[1:2, :] * prod_s[lo : lo + BLOCK, :]
            + conv_ref[2:3, :] * prod_s[lo + 1 : lo + 1 + BLOCK, :]
        )
        act_s[at : at + BLOCK, 256:512] = (p_s[rows, 384:640].astype(jnp.float32) * mixed).astype(
            jnp.bfloat16
        )

    for lo in range(0, features, 256):
        out_ref[:, lo : lo + 256] = lax.dot_general(
            act_s[...],
            w_s[lo : lo + 256, PROJ:],
            (((1,), (1,)), ((), ())),
            preferred_element_type=jnp.float32,
        ).astype(jnp.bfloat16)


def run_layer(where, sinks, tokens, pieces, tables, conv):
    features = tokens.shape[-1]
    return pl.pallas_call(
        layer_kernel,
        out_shape=jax.ShapeDtypeStruct((MAIN, features), jnp.bfloat16),
        in_specs=[SMEM, SMEM] + [VMEM] * (1 + len(pieces) + len(tables) + 1),
        out_specs=VMEM,
        scratch_shapes=[
            pltpu.VMEM((features, WIDTH), jnp.bfloat16),
            pltpu.VMEM((ROWS, PROJ), jnp.bfloat16),
            pltpu.VMEM((ROWS, 128), jnp.bfloat16),
            pltpu.VMEM((ROWS, 128), jnp.bfloat16),
            pltpu.VMEM((ROWS, 256), jnp.float32),
            pltpu.VMEM((MAIN, 512), jnp.bfloat16),
        ],
        compiler_params=pltpu.CompilerParams(vmem_limit_bytes=32 * MIB),
        name="layer",
    )(where, sinks, tokens, *pieces, *tables, conv)


def per_device(
    tokens,
    norm_gain,
    query_weight,
    key_weight,
    value_weight,
    gate_weight,
    left_weight,
    input_weight,
    query_gain,
    key_gain,
    sink_logit,
    conv_weight,
    out_attention,
    out_conv,
):
    place = lax.axis_index("sp").astype(jnp.int32)
    where = jnp.stack([lax.rem(place, 2), lax.rem(place // 2, RING), place // (2 * RING), place])
    gathered = gathered_tokens(normalized(tokens, norm_gain))
    pieces = gathered_weights(
        (
            query_weight,
            key_weight,
            value_weight,
            gate_weight,
            left_weight,
            input_weight,
            out_attention,
            out_conv,
        )
    )
    positions = (place * MAIN - WINDOW + jnp.arange(ROWS, dtype=jnp.int32)).astype(jnp.float32)
    angle = positions[:, None] * ANGLES
    tables = (jnp.cos(angle), jnp.sin(angle), query_gain[None], key_gain[None])
    partial = run_layer(where, sink_logit, gathered, pieces, tables, conv_weight)
    blocks = lax.all_to_all(partial.reshape(TP, LOCAL, -1), "tp", 0, 0, tiled=True)
    return blocks.astype(jnp.float32).sum(axis=0).astype(jnp.bfloat16)


def solution(mesh):
    in_specs = (
        P(("sp", "tp"), None),
        P(),
        P("tp", "sp"),
        P("tp", "sp"),
        P("tp", "sp"),
        P("tp", "sp"),
        P("tp", "sp"),
        P("tp", "sp"),
        P(),
        P(),
        P("tp"),
        P(None, "tp"),
        P("tp", "sp"),
        P("tp", "sp"),
    )
    out_specs = P(("sp", "tp"), None)

    return jax.shard_map(
        per_device, mesh=mesh, in_specs=in_specs, out_specs=out_specs, check_vma=False
    )
```

```python
import jax
import jax.numpy as jnp
import numpy as np
from jax import lax
from jax.experimental import pallas as pl
from jax.experimental.pallas import tpu as pltpu
from jax.sharding import PartitionSpec as P


HEAD = 64
HALF = HEAD // 2
WINDOW = 128
BLOCK = 128
EPS = 1e-06
ROPE_BASE = 10000.0
NEG_FILL = -1e30
RING = 8
TP = 4
CHIPS = RING * RING
SP = 2 * CHIPS
LOCAL = 64
MAIN = TP * LOCAL
ROWS = MAIN + 2 * WINDOW
SHARE = 2 * LOCAL
PROJ = 1152
WIDTH = PROJ + 512


def sp_of(z, y, c):
    return (z * RING + y) * 2 + c


def even_partner(pos):
    return pos ^ 1


def odd_partner(pos):
    return (pos - 1) % RING if pos % 2 == 0 else (pos + 1) % RING


def matching(partner):
    pairs = []
    for z in range(RING):
        for y in range(RING):
            pairs.append((sp_of(z, y, 0), sp_of(z, partner(y), 0)))
            pairs.append((sp_of(z, y, 1), sp_of(partner(z), y, 1)))
    return pairs


EVEN = matching(even_partner)
ODD = matching(odd_partner)
SWAP = [(2 * k + c, 2 * k + 1 - c) for k in range(CHIPS) for c in range(2)]
GROUPS = [[sp_of(z, y, 0) for z in range(RING)] for y in range(RING)] + [
    [sp_of(z, y, 1) for y in range(RING)] for z in range(RING)
]
HALO = [(s * TP + x, (s + 1) * TP + x) for s in range(SP - 1) for x in (2, 3)] + [
    ((s + 1) * TP + x, s * TP + x) for s in range(SP - 1) for x in (0, 1)
]
MIB = 1024 * 1024
ANGLES = np.tile(ROPE_BASE ** (-np.arange(HALF) / HALF), 128 // HALF).astype(np.float32)
VMEM = pl.BlockSpec(memory_space=pltpu.VMEM)
SMEM = pl.BlockSpec(memory_space=pltpu.SMEM)


def copies_kernel(*refs):
    *weights, out = refs
    at = 0
    for ref in weights:
        width = ref.shape[1]
        for k in range(RING):
            out[k, :, at : at + width] = ref[...]
        at += width


def copies(weights):
    return pl.pallas_call(
        copies_kernel,
        out_shape=jax.ShapeDtypeStruct((RING, weights[0].shape[1], WIDTH), jnp.bfloat16),
        in_specs=[VMEM] * len(weights),
        out_specs=VMEM,
        name="copies",
    )(*[w.T for w in weights])


def rows_kernel(normed, rim, out):
    for x in range(TP):
        out[x, :LOCAL, :] = normed[...]
        out[x, LOCAL:, :] = rim[...]


def row_copies(normed, rim):
    return pl.pallas_call(
        rows_kernel,
        out_shape=jax.ShapeDtypeStruct((TP, SHARE, normed.shape[1]), jnp.bfloat16),
        in_specs=[VMEM] * 2,
        out_specs=VMEM,
        compiler_params=pltpu.CompilerParams(vmem_limit_bytes=8 * MIB),
    name="rows",
    )(normed, rim)


def gathered_weights(weights):
    blocks = copies(weights)
    own = lax.all_to_all(blocks, "sp", 0, 0, axis_index_groups=GROUPS, tiled=True)
    own = own.reshape(-1, WIDTH)
    e1 = lax.ppermute(own, "sp", EVEN)
    o1 = lax.ppermute(own, "sp", ODD)
    o2 = lax.ppermute(e1, "sp", ODD)
    e2 = lax.ppermute(o1, "sp", EVEN)
    e3 = lax.ppermute(o2, "sp", EVEN)
    o3 = lax.ppermute(e2, "sp", ODD)
    o4 = lax.ppermute(e3, "sp", ODD)
    first = packed((own, e1, o1, o2))
    second = packed((e2, e3, o3))
    kept = (first, second, o4)
    return kept + tuple(lax.ppermute(p, "sp", SWAP) for p in kept)


def packed(pieces):
    def body(*refs):
        *sources, out = refs
        for k, ref in enumerate(sources):
            out[k * 128 : (k + 1) * 128, :] = ref[...]

    return pl.pallas_call(
        body,
        out_shape=jax.ShapeDtypeStruct((128 * len(pieces), WIDTH), jnp.bfloat16),
        in_specs=[VMEM] * len(pieces),
        out_specs=VMEM,
        compiler_params=pltpu.CompilerParams(vmem_limit_bytes=8 * MIB),
    )(*pieces)


def norm_kernel(x_ref, gain_ref, normed):
    wide = x_ref[...].astype(jnp.float32)
    mean = jnp.mean(wide * wide, axis=-1, keepdims=True)
    normed[...] = (wide * lax.rsqrt(mean + EPS) * gain_ref[...]).astype(jnp.bfloat16)


def normalized(tokens, norm_gain):
    return pl.pallas_call(
        norm_kernel,
        out_shape=jax.ShapeDtypeStruct(tokens.shape, jnp.bfloat16),
        in_specs=[VMEM] * 2,
        out_specs=VMEM,
        name="norm",
    )(tokens, norm_gain[None])


def gathered_tokens(normed):
    rim = lax.ppermute(normed, ("sp", "tp"), HALO)
    sent = row_copies(normed, rim)
    return lax.all_to_all(sent, "tp", 0, 0, tiled=True)


PIECE_STEPS = (0, 1, -1, -2, 2, 3, -3, -4)


def layer_kernel(where_ref, sink_ref, x_ref, *refs):
    pieces = []
    for first, second, third in (refs[:3], refs[3:6]):
        pieces += [(first, k * 128) for k in range(4)]
        pieces += [(second, k * 128) for k in range(3)] + [(third, 0)]
    turn_ref, qg_ref, kg_ref, conv_ref, out_ref = refs[6:11]
    w_s, p_s, kv_s, kk_s, vv_s, prod_s, act_s = refs[11:]
    core, y, z, place = where_ref[0], where_ref[1], where_ref[2], where_ref[3]

    for k, (piece, base) in enumerate(pieces):
        owner = core if k < 8 else 1 - core
        pos = jnp.where(owner == 0, y, z)
        sgn = 1 - 2 * lax.rem(pos, 2)
        at = lax.rem(pos + sgn * PIECE_STEPS[k % 8] + 2 * RING, RING)
        for j in range(RING):
            to = jnp.where(owner == 0, j * 256 + at * 32, at * 256 + j * 32 + 16)
            w_s[pl.ds(pl.multiple_of(to, 16), 16), :] = piece[
                base + j * 16 : base + (j + 1) * 16, :
            ]

    features = x_ref.shape[-1]
    raw = x_ref[...].reshape(ROWS, features)
    pairs = jnp.dot(raw, w_s[:, 256:384], preferred_element_type=jnp.float32).astype(jnp.bfloat16)
    for x in range(TP):
        base = x * SHARE
        kv_s[WINDOW + x * LOCAL : WINDOW + (x + 1) * LOCAL, :] = pairs[base : base + LOCAL]
        to = (x - 2) * LOCAL if x >= 2 else WINDOW + MAIN + x * LOCAL
        kv_s[to : to + LOCAL, :] = pairs[base + LOCAL : base + SHARE]

    edges = [x_ref[TP - 1, SHARE - 8 :, :], x_ref[0, LOCAL : LOCAL + 8, :]]
    main = jnp.concatenate([x_ref[:, :LOCAL, :].reshape(MAIN, features)] + edges, axis=0)
    for lo in (0, 384, 640, 896):
        part = jnp.dot(main, w_s[:, lo : lo + 256], preferred_element_type=jnp.float32)
        p_s[:, lo : lo + 256] = part.astype(jnp.bfloat16)

    def gain_rows(ref, scale):
        gain = jnp.concatenate([ref[...], ref[...]], axis=1) * scale
        lane = lax.rem(lax.broadcasted_iota(jnp.int32, gain.shape, 1), HEAD)
        low = pltpu.roll(gain, 128 - HALF, 1)
        return gain, jnp.where(lane < HALF, -low, pltpu.roll(gain, HALF, 1))

    query_gain = gain_rows(qg_ref, HEAD ** (-0.5))
    key_gain = gain_rows(kg_ref, 1.0)

    def rotated(value, at, gain, crossed_gain):
        lane = lax.broadcasted_iota(jnp.int32, value.shape, 1)
        low = lane < HEAD
        square = value * value
        mean0 = jnp.sum(jnp.where(low, square, 0.0), axis=-1, keepdims=True) * (1.0 / HEAD)
        mean1 = jnp.sum(jnp.where(low, 0.0, square), axis=-1, keepdims=True) * (1.0 / HEAD)
        scaled = value * jnp.where(low, lax.rsqrt(mean0 + EPS), lax.rsqrt(mean1 + EPS))
        crossed = jnp.where(
            lax.rem(lane, HEAD) < HALF,
            pltpu.roll(scaled, 2 * HEAD - HALF, 1),
            pltpu.roll(scaled, HALF, 1),
        )
        row = BLOCK + at // BLOCK
        cos0, sin0 = turn_ref[0, row : row + 1, :], turn_ref[1, row : row + 1, :]
        cos1, sin1 = turn_ref[0, :BLOCK, :], turn_ref[1, :BLOCK, :]
        cosine = cos0 * cos1 - sin0 * sin1
        sine = sin0 * cos1 + cos0 * sin1
        return scaled * (cosine * gain) + crossed * (sine * crossed_gain)

    for at in range(0, ROWS, BLOCK):
        kv = kv_s[at : at + BLOCK, :].astype(jnp.float32)
        lane = lax.broadcasted_iota(jnp.int32, kv.shape, 1)
        key = rotated(kv, at, *key_gain)
        kk_s[at : at + BLOCK, :] = jnp.where(lane < HEAD, key, pltpu.roll(key, HEAD, 1)).astype(
            jnp.bfloat16
        )
        vv_s[at : at + BLOCK, :] = jnp.where(lane < HEAD, pltpu.roll(kv, HEAD, 1), kv).astype(
            jnp.bfloat16
        )

    product = p_s[:, 640:896].astype(jnp.float32) * p_s[:, 896:1152].astype(jnp.float32)
    product = product.astype(jnp.bfloat16).astype(jnp.float32)
    prod_s[8 : 8 + MAIN, :] = product[:MAIN]
    prod_s[:8, :] = product[MAIN : MAIN + 8]
    prod_s[8 + MAIN :, :] = product[MAIN + 8 :]

    for at in range(0, MAIN, BLOCK):
        rows = slice(at, at + BLOCK)
        keys = kk_s[at : at + 3 * BLOCK, :]
        values = vv_s[at : at + 3 * BLOCK, :]
        shape = (BLOCK, 3 * BLOCK)
        q_at = lax.broadcasted_iota(jnp.int32, shape, 0)
        k_at = lax.broadcasted_iota(jnp.int32, shape, 1) - WINDOW
        k_pos = k_at + (place * MAIN + at)
        allowed = (jnp.abs(q_at - k_at) <= WINDOW) & (k_pos >= 0) & (k_pos < SP * MAIN)
        low = lax.broadcasted_iota(jnp.int32, (BLOCK, 128), 1) < HEAD
        queries = []
        for pair in range(2):
            lanes = slice(pair * 128, (pair + 1) * 128)
            query = rotated(p_s[rows, lanes].astype(jnp.float32), at + WINDOW, *query_gain)
            queries += [jnp.where(low, query, 0.0), jnp.where(low, 0.0, query)]
        stacked = jnp.concatenate(queries, axis=0).astype(jnp.bfloat16)
        scores = lax.dot_general(
            stacked, keys, (((1,), (1,)), ((), ())), preferred_element_type=jnp.float32
        )
        weights = []
        for head in range(4):
            score = jnp.where(allowed, scores[head * BLOCK : (head + 1) * BLOCK], NEG_FILL)
            sink = sink_ref[head]
            top = jnp.maximum(jnp.max(score, axis=-1, keepdims=True), sink)
            expo = jnp.exp(score - top)
            total = jnp.sum(expo, axis=-1, keepdims=True) + jnp.exp(sink - top)
            weights.append((expo * (1.0 / total)).astype(jnp.bfloat16))
        outs = jnp.dot(
            jnp.concatenate(weights, axis=0), values, preferred_element_type=jnp.float32
        ).astype(jnp.bfloat16)
        for pair in range(2):
            first = outs[2 * pair * BLOCK : (2 * pair + 1) * BLOCK]
            second = outs[(2 * pair + 1) * BLOCK : (2 * pair + 2) * BLOCK]
            act_s[rows, pair * 128 : (pair + 1) * 128] = jnp.where(low, first, second)
        lo = at + 8
        mixed = (
            conv_ref[0:1, :] * prod_s[lo - 1 : lo - 1 + BLOCK, :]
            + conv_ref[1:2, :] * prod_s[lo : lo + BLOCK, :]
            + conv_ref[2:3, :] * prod_s[lo + 1 : lo + 1 + BLOCK, :]
        )
        act_s[rows, 256:512] = (p_s[rows, 384:640].astype(jnp.float32) * mixed).astype(
            jnp.bfloat16
        )

    for lo in range(0, features, 256):
        out_ref[:, lo : lo + 256] = lax.dot_general(
            act_s[...],
            w_s[lo : lo + 256, PROJ:],
            (((1,), (1,)), ((), ())),
            preferred_element_type=jnp.float32,
        ).astype(jnp.bfloat16)


def run_layer(where, sinks, tokens, pieces, tables, conv):
    features = tokens.shape[-1]
    return pl.pallas_call(
        layer_kernel,
        out_shape=jax.ShapeDtypeStruct((MAIN, features), jnp.bfloat16),
        in_specs=[SMEM, SMEM] + [VMEM] * (1 + len(pieces) + len(tables) + 1),
        out_specs=VMEM,
        scratch_shapes=[
            pltpu.VMEM((features, WIDTH), jnp.bfloat16),
            pltpu.VMEM((MAIN + 16, PROJ), jnp.bfloat16),
            pltpu.VMEM((ROWS, 128), jnp.bfloat16),
            pltpu.VMEM((ROWS, 128), jnp.bfloat16),
            pltpu.VMEM((ROWS, 128), jnp.bfloat16),
            pltpu.VMEM((MAIN + 16, 256), jnp.float32),
            pltpu.VMEM((MAIN, 512), jnp.bfloat16),
        ],
        compiler_params=pltpu.CompilerParams(vmem_limit_bytes=32 * MIB),
        name="layer",
    )(where, sinks, tokens, *pieces, *tables, conv)


def per_device(
    tokens,
    norm_gain,
    query_weight,
    key_weight,
    value_weight,
    gate_weight,
    left_weight,
    input_weight,
    query_gain,
    key_gain,
    sink_logit,
    conv_weight,
    out_attention,
    out_conv,
):
    place = lax.axis_index("sp").astype(jnp.int32)
    where = jnp.stack([lax.rem(place, 2), lax.rem(place // 2, RING), place // (2 * RING), place])
    gathered = gathered_tokens(normalized(tokens, norm_gain))
    pieces = gathered_weights(
        (
            query_weight,
            key_weight,
            value_weight,
            gate_weight,
            left_weight,
            input_weight,
            out_attention,
            out_conv,
        )
    )
    starts = place * MAIN - WINDOW + BLOCK * jnp.arange(8, dtype=jnp.int32)
    rows = jnp.concatenate([jnp.arange(BLOCK, dtype=jnp.int32), starts]).astype(jnp.float32)
    angle = rows[:, None] * ANGLES
    turns = jnp.stack([jnp.cos(angle), jnp.sin(angle)])
    tables = (turns, query_gain[None], key_gain[None])
    partial = run_layer(where, sink_logit, gathered, pieces, tables, conv_weight)
    blocks = lax.all_to_all(partial.reshape(TP, LOCAL, -1), "tp", 0, 0, tiled=True)
    return blocks.astype(jnp.float32).sum(axis=0).astype(jnp.bfloat16)


def solution(mesh):
    in_specs = (
        P(("sp", "tp"), None),
        P(),
        P("tp", "sp"),
        P("tp", "sp"),
        P("tp", "sp"),
        P("tp", "sp"),
        P("tp", "sp"),
        P("tp", "sp"),
        P(),
        P(),
        P("tp"),
        P(None, "tp"),
        P("tp", "sp"),
        P("tp", "sp"),
    )
    out_specs = P(("sp", "tp"), None)

    return jax.shard_map(
        per_device, mesh=mesh, in_specs=in_specs, out_specs=out_specs, check_vma=False
    )
```

```python
import jax
import jax.numpy as jnp
import numpy as np
from jax import lax
from jax.experimental import pallas as pl
from jax.experimental.pallas import tpu as pltpu
from jax.sharding import PartitionSpec as P


HEAD = 64
HALF = HEAD // 2
WINDOW = 128
BLOCK = 128
EPS = 1e-06
ROPE_BASE = 10000.0
NEG_FILL = -1e30
RING = 8
TP = 4
CHIPS = RING * RING
SP = 2 * CHIPS
LOCAL = 64
MAIN = TP * LOCAL
ROWS = MAIN + 2 * WINDOW
SHARE = 2 * LOCAL
PROJ = 1152
WIDTH = PROJ + 512


def sp_of(z, y, c):
    return (z * RING + y) * 2 + c


def even_partner(pos):
    return pos ^ 1


def odd_partner(pos):
    return (pos - 1) % RING if pos % 2 == 0 else (pos + 1) % RING


def matching(partner):
    pairs = []
    for z in range(RING):
        for y in range(RING):
            pairs.append((sp_of(z, y, 0), sp_of(z, partner(y), 0)))
            pairs.append((sp_of(z, y, 1), sp_of(partner(z), y, 1)))
    return pairs


def two_away(pos):
    return (pos + 2) % RING if pos % 2 == 0 else (pos - 2) % RING


EVEN = matching(even_partner)
ODD = matching(odd_partner)
FAR = matching(two_away)
SWAP = [(2 * k + c, 2 * k + 1 - c) for k in range(CHIPS) for c in range(2)]
GROUPS = [[sp_of(z, y, 0) for z in range(RING)] for y in range(RING)] + [
    [sp_of(z, y, 1) for y in range(RING)] for z in range(RING)
]
HALO = [(s * TP + x, (s + 1) * TP + x) for s in range(SP - 1) for x in (2, 3)] + [
    ((s + 1) * TP + x, s * TP + x) for s in range(SP - 1) for x in (0, 1)
]
MIB = 1024 * 1024
ANGLES = np.tile(ROPE_BASE ** (-np.arange(HALF) / HALF), 128 // HALF).astype(np.float32)
VMEM = pl.BlockSpec(memory_space=pltpu.VMEM)
SMEM = pl.BlockSpec(memory_space=pltpu.SMEM)


def copies_kernel(*refs):
    *weights, out = refs
    at = 0
    for ref in weights:
        width = ref.shape[1]
        for k in range(RING):
            out[k, :, at : at + width] = ref[...]
        at += width


def copies(weights):
    return pl.pallas_call(
        copies_kernel,
        out_shape=jax.ShapeDtypeStruct((RING, weights[0].shape[1], WIDTH), jnp.bfloat16),
        in_specs=[VMEM] * len(weights),
        out_specs=VMEM,
        name="copies",
    )(*[w.T for w in weights])


def rows_kernel(normed, rim, out):
    for x in range(TP):
        out[x, :LOCAL, :] = normed[...]
        out[x, LOCAL:, :] = rim[...]


def row_copies(normed, rim):
    return pl.pallas_call(
        rows_kernel,
        out_shape=jax.ShapeDtypeStruct((TP, SHARE, normed.shape[1]), jnp.bfloat16),
        in_specs=[VMEM] * 2,
        out_specs=VMEM,
        compiler_params=pltpu.CompilerParams(vmem_limit_bytes=8 * MIB),
    name="rows",
    )(normed, rim)


def gathered_weights(weights):
    blocks = copies(weights)
    own = lax.all_to_all(blocks, "sp", 0, 0, axis_index_groups=GROUPS, tiled=True)
    own = own.reshape(-1, WIDTH)
    e1 = lax.ppermute(own, "sp", EVEN)
    o1 = lax.ppermute(own, "sp", ODD)
    o2 = lax.ppermute(e1, "sp", ODD)
    e2 = lax.ppermute(o1, "sp", EVEN)
    e3 = lax.ppermute(o2, "sp", EVEN)
    o3 = lax.ppermute(e2, "sp", ODD)
    f4 = lax.ppermute(o2, "sp", FAR)
    first = packed((own, e1, o1, o2))
    second = packed((e2, e3))
    kept = (first, second, f4, o3)
    return kept + tuple(lax.ppermute(p, "sp", SWAP) for p in kept)


def packed(pieces):
    def body(*refs):
        *sources, out = refs
        for k, ref in enumerate(sources):
            out[k * 128 : (k + 1) * 128, :] = ref[...]

    return pl.pallas_call(
        body,
        out_shape=jax.ShapeDtypeStruct((128 * len(pieces), WIDTH), jnp.bfloat16),
        in_specs=[VMEM] * len(pieces),
        out_specs=VMEM,
        compiler_params=pltpu.CompilerParams(vmem_limit_bytes=8 * MIB),
    )(*pieces)


def norm_kernel(x_ref, gain_ref, normed):
    wide = x_ref[...].astype(jnp.float32)
    mean = jnp.mean(wide * wide, axis=-1, keepdims=True)
    normed[...] = (wide * lax.rsqrt(mean + EPS) * gain_ref[...]).astype(jnp.bfloat16)


def normalized(tokens, norm_gain):
    return pl.pallas_call(
        norm_kernel,
        out_shape=jax.ShapeDtypeStruct(tokens.shape, jnp.bfloat16),
        in_specs=[VMEM] * 2,
        out_specs=VMEM,
        name="norm",
    )(tokens, norm_gain[None])


def gathered_tokens(normed):
    rim = lax.ppermute(normed, ("sp", "tp"), HALO)
    sent = row_copies(normed, rim)
    return lax.all_to_all(sent, "tp", 0, 0, tiled=True)


PIECE_STEPS = (0, 1, -1, -2, 2, 3, 4, -3)


def layer_kernel(where_ref, sink_ref, x_ref, *refs):
    pieces = []
    for first, second, third, fourth in (refs[:4], refs[4:8]):
        pieces += [(first, k * 128) for k in range(4)]
        pieces += [(second, 0), (second, 128), (third, 0), (fourth, 0)]
    turn_ref, qg_ref, kg_ref, conv_ref, out_ref = refs[8:13]
    w_s, p_s, kv_s, kk_s, vv_s, prod_s, act_s = refs[13:]
    core, y, z, place = where_ref[0], where_ref[1], where_ref[2], where_ref[3]

    for k, (piece, base) in enumerate(pieces):
        owner = core if k < 8 else 1 - core
        pos = jnp.where(owner == 0, y, z)
        sgn = 1 - 2 * lax.rem(pos, 2)
        at = lax.rem(pos + sgn * PIECE_STEPS[k % 8] + 2 * RING, RING)
        for j in range(RING):
            to = jnp.where(owner == 0, j * 256 + at * 32, at * 256 + j * 32 + 16)
            w_s[pl.ds(pl.multiple_of(to, 16), 16), :] = piece[
                base + j * 16 : base + (j + 1) * 16, :
            ]

    features = x_ref.shape[-1]
    raw = x_ref[...].reshape(ROWS, features)
    pairs = jnp.dot(raw, w_s[:, 256:384], preferred_element_type=jnp.float32).astype(jnp.bfloat16)
    for x in range(TP):
        base = x * SHARE
        kv_s[WINDOW + x * LOCAL : WINDOW + (x + 1) * LOCAL, :] = pairs[base : base + LOCAL]
        to = (x - 2) * LOCAL if x >= 2 else WINDOW + MAIN + x * LOCAL
        kv_s[to : to + LOCAL, :] = pairs[base + LOCAL : base + SHARE]

    edges = [x_ref[TP - 1, SHARE - 8 :, :], x_ref[0, LOCAL : LOCAL + 8, :]]
    main = jnp.concatenate([x_ref[:, :LOCAL, :].reshape(MAIN, features)] + edges, axis=0)
    for lo in (0, 384, 640, 896):
        part = jnp.dot(main, w_s[:, lo : lo + 256], preferred_element_type=jnp.float32)
        p_s[:, lo : lo + 256] = part.astype(jnp.bfloat16)

    def gain_rows(ref, scale):
        gain = jnp.concatenate([ref[...], ref[...]], axis=1) * scale
        lane = lax.rem(lax.broadcasted_iota(jnp.int32, gain.shape, 1), HEAD)
        low = pltpu.roll(gain, 128 - HALF, 1)
        return gain, jnp.where(lane < HALF, -low, pltpu.roll(gain, HALF, 1))

    query_gain = gain_rows(qg_ref, HEAD ** (-0.5))
    key_gain = gain_rows(kg_ref, 1.0)

    def rotated(value, at, gain, crossed_gain):
        lane = lax.broadcasted_iota(jnp.int32, value.shape, 1)
        low = lane < HEAD
        square = value * value
        mean0 = jnp.sum(jnp.where(low, square, 0.0), axis=-1, keepdims=True) * (1.0 / HEAD)
        mean1 = jnp.sum(jnp.where(low, 0.0, square), axis=-1, keepdims=True) * (1.0 / HEAD)
        scaled = value * jnp.where(low, lax.rsqrt(mean0 + EPS), lax.rsqrt(mean1 + EPS))
        crossed = jnp.where(
            lax.rem(lane, HEAD) < HALF,
            pltpu.roll(scaled, 2 * HEAD - HALF, 1),
            pltpu.roll(scaled, HALF, 1),
        )
        row = BLOCK + at // BLOCK
        cos0, sin0 = turn_ref[0, row : row + 1, :], turn_ref[1, row : row + 1, :]
        cos1, sin1 = turn_ref[0, :BLOCK, :], turn_ref[1, :BLOCK, :]
        cosine = cos0 * cos1 - sin0 * sin1
        sine = sin0 * cos1 + cos0 * sin1
        return scaled * (cosine * gain) + crossed * (sine * crossed_gain)

    for at in range(0, ROWS, BLOCK):
        kv = kv_s[at : at + BLOCK, :].astype(jnp.float32)
        lane = lax.broadcasted_iota(jnp.int32, kv.shape, 1)
        key = rotated(kv, at, *key_gain)
        kk_s[at : at + BLOCK, :] = jnp.where(lane < HEAD, key, pltpu.roll(key, HEAD, 1)).astype(
            jnp.bfloat16
        )
        vv_s[at : at + BLOCK, :] = jnp.where(lane < HEAD, pltpu.roll(kv, HEAD, 1), kv).astype(
            jnp.bfloat16
        )

    product = p_s[:, 640:896].astype(jnp.float32) * p_s[:, 896:1152].astype(jnp.float32)
    product = product.astype(jnp.bfloat16).astype(jnp.float32)
    prod_s[8 : 8 + MAIN, :] = product[:MAIN]
    prod_s[:8, :] = product[MAIN : MAIN + 8]
    prod_s[8 + MAIN :, :] = product[MAIN + 8 :]

    for at in range(0, MAIN, BLOCK):
        rows = slice(at, at + BLOCK)
        keys = kk_s[at : at + 3 * BLOCK, :]
        values = vv_s[at : at + 3 * BLOCK, :]
        shape = (BLOCK, 3 * BLOCK)
        q_at = lax.broadcasted_iota(jnp.int32, shape, 0)
        k_at = lax.broadcasted_iota(jnp.int32, shape, 1) - WINDOW
        k_pos = k_at + (place * MAIN + at)
        allowed = (jnp.abs(q_at - k_at) <= WINDOW) & (k_pos >= 0) & (k_pos < SP * MAIN)
        low = lax.broadcasted_iota(jnp.int32, (BLOCK, 128), 1) < HEAD
        queries = []
        for pair in range(2):
            lanes = slice(pair * 128, (pair + 1) * 128)
            query = rotated(p_s[rows, lanes].astype(jnp.float32), at + WINDOW, *query_gain)
            queries += [jnp.where(low, query, 0.0), jnp.where(low, 0.0, query)]
        stacked = jnp.concatenate(queries, axis=0).astype(jnp.bfloat16)
        scores = lax.dot_general(
            stacked, keys, (((1,), (1,)), ((), ())), preferred_element_type=jnp.float32
        )
        weights = []
        for head in range(4):
            score = jnp.where(allowed, scores[head * BLOCK : (head + 1) * BLOCK], NEG_FILL)
            sink = sink_ref[head]
            top = jnp.maximum(jnp.max(score, axis=-1, keepdims=True), sink)
            expo = jnp.exp(score - top)
            total = jnp.sum(expo, axis=-1, keepdims=True) + jnp.exp(sink - top)
            weights.append((expo * (1.0 / total)).astype(jnp.bfloat16))
        outs = jnp.dot(
            jnp.concatenate(weights, axis=0), values, preferred_element_type=jnp.float32
        ).astype(jnp.bfloat16)
        for pair in range(2):
            first = outs[2 * pair * BLOCK : (2 * pair + 1) * BLOCK]
            second = outs[(2 * pair + 1) * BLOCK : (2 * pair + 2) * BLOCK]
            act_s[rows, pair * 128 : (pair + 1) * 128] = jnp.where(low, first, second)
        lo = at + 8
        mixed = (
            conv_ref[0:1, :] * prod_s[lo - 1 : lo - 1 + BLOCK, :]
            + conv_ref[1:2, :] * prod_s[lo : lo + BLOCK, :]
            + conv_ref[2:3, :] * prod_s[lo + 1 : lo + 1 + BLOCK, :]
        )
        act_s[rows, 256:512] = (p_s[rows, 384:640].astype(jnp.float32) * mixed).astype(
            jnp.bfloat16
        )

    for lo in range(0, features, 256):
        out_ref[:, lo : lo + 256] = lax.dot_general(
            act_s[...],
            w_s[lo : lo + 256, PROJ:],
            (((1,), (1,)), ((), ())),
            preferred_element_type=jnp.float32,
        ).astype(jnp.bfloat16)


def run_layer(where, sinks, tokens, pieces, tables, conv):
    features = tokens.shape[-1]
    return pl.pallas_call(
        layer_kernel,
        out_shape=jax.ShapeDtypeStruct((MAIN, features), jnp.bfloat16),
        in_specs=[SMEM, SMEM] + [VMEM] * (1 + len(pieces) + len(tables) + 1),
        out_specs=VMEM,
        scratch_shapes=[
            pltpu.VMEM((features, WIDTH), jnp.bfloat16),
            pltpu.VMEM((MAIN + 16, PROJ), jnp.bfloat16),
            pltpu.VMEM((ROWS, 128), jnp.bfloat16),
            pltpu.VMEM((ROWS, 128), jnp.bfloat16),
            pltpu.VMEM((ROWS, 128), jnp.bfloat16),
            pltpu.VMEM((MAIN + 16, 256), jnp.float32),
            pltpu.VMEM((MAIN, 512), jnp.bfloat16),
        ],
        compiler_params=pltpu.CompilerParams(vmem_limit_bytes=32 * MIB),
        name="layer",
    )(where, sinks, tokens, *pieces, *tables, conv)


def per_device(
    tokens,
    norm_gain,
    query_weight,
    key_weight,
    value_weight,
    gate_weight,
    left_weight,
    input_weight,
    query_gain,
    key_gain,
    sink_logit,
    conv_weight,
    out_attention,
    out_conv,
):
    place = lax.axis_index("sp").astype(jnp.int32)
    where = jnp.stack([lax.rem(place, 2), lax.rem(place // 2, RING), place // (2 * RING), place])
    gathered = gathered_tokens(normalized(tokens, norm_gain))
    pieces = gathered_weights(
        (
            query_weight,
            key_weight,
            value_weight,
            gate_weight,
            left_weight,
            input_weight,
            out_attention,
            out_conv,
        )
    )
    starts = place * MAIN - WINDOW + BLOCK * jnp.arange(8, dtype=jnp.int32)
    rows = jnp.concatenate([jnp.arange(BLOCK, dtype=jnp.int32), starts]).astype(jnp.float32)
    angle = rows[:, None] * ANGLES
    turns = jnp.stack([jnp.cos(angle), jnp.sin(angle)])
    tables = (turns, query_gain[None], key_gain[None])
    partial = run_layer(where, sink_logit, gathered, pieces, tables, conv_weight)
    blocks = lax.all_to_all(partial.reshape(TP, LOCAL, -1), "tp", 0, 0, tiled=True)
    return blocks.astype(jnp.float32).sum(axis=0).astype(jnp.bfloat16)


def solution(mesh):
    in_specs = (
        P(("sp", "tp"), None),
        P(),
        P("tp", "sp"),
        P("tp", "sp"),
        P("tp", "sp"),
        P("tp", "sp"),
        P("tp", "sp"),
        P("tp", "sp"),
        P(),
        P(),
        P("tp"),
        P(None, "tp"),
        P("tp", "sp"),
        P("tp", "sp"),
    )
    out_specs = P(("sp", "tp"), None)

    return jax.shard_map(
        per_device, mesh=mesh, in_specs=in_specs, out_specs=out_specs, check_vma=False
    )
```
